1024 devices in a mesh: grp: 2 (over x), tp: 16 (over z), dp: 32 (over y, core).
Axes of the slice: x: 2, y: 16, z: 16, core: 2. Of those that a mesh axis runs over, the one named last changes fastest.
The devices are a block of a 4x16x16 slice.
Arguments:
- tokens: bfloat16 [256, 4096], P(('grp', 'tp'), 'dp'), parts along dimension 0, may hold values from -30 to 30
- norm_gain: float32 [2, 4096], P(None, 'dp'), may hold values from 0.1 to 1.9
- w_query: bfloat16 [2, 4096, 2048], P(None, 'dp', 'tp'), may hold values from -0.09375 to 0.09375
- w_forget: bfloat16 [2, 4096, 2048], P(None, 'dp', 'tp'), may hold values from -0.09375 to 0.09375
- w_value: bfloat16 [2, 4096, 2048], P(None, 'dp', 'tp'), may hold values from -0.09375 to 0.09375
- w_gate: bfloat16 [2, 4096, 2048], P(None, 'dp', 'tp'), may hold values from -0.09375 to 0.09375
- lower_bound: float32 [2, 2048], P(None, 'tp'), may hold values from 0 to 0.9
- head_gain: float32 [2, 128], replicated, may hold values from 0.1 to 1.9
- w_out: bfloat16 [2, 2048, 4096], P(None, 'tp', 'dp'), may hold values from -0.125 to 0.125
- state: float32 [2, 256, 16, 128, 128], P(None, ('grp', 'dp'), 'tp'), parts along dimension 1, may hold values from -4 to 4
Outputs:
- hidden_out: bfloat16 [256, 4096], P(('grp', 'tp'), 'dp'), parts along dimension 0
- new_state: float32 [2, 256, 16, 128, 128], P(None, ('grp', 'dp'), 'tp'), parts along dimension 1
The draws below stay inside these ranges and needn't reach their ends.
There are 2 independent parts, one for each index of `grp`. The reference program is written for one: setup_inputs(seed, part) draws one part's arguments, and reference() takes and returns one part's arrays. A program takes and returns all parts, laid end to end along the dimension named above; an argument that names none is the same for every part. Nothing has to cross between parts.
All inputs are finite; a program needn't handle non-finite values.
Results may differ from the reference program's by a relative error of at most 0.02.
Values may be sent and summed in bfloat16 or wider, within the bound.
No kernel may reach another device: no remote copies, remote signals or barrier semaphores. Data moves between devices by JAX's collectives and lax.ppermute only.
A program may use at most 32 MiB of HBM per device.

```python
import jax
import jax.numpy as jnp
from jax import lax

D = 4096
HEADS = 16
HD = 128
DH = 2048
BATCH = 128


def draw_tokens(key, part):
    first_key, second_key = jax.random.split(key, 2)
    column_scale = jnp.repeat(jnp.exp(jax.random.uniform(second_key, (D // 16,), jnp.float32, -1.2, 1.2)), 16)
    values = jax.random.normal(first_key, (BATCH, D), jnp.float32) * column_scale
    return jnp.clip(values, -30.0, 30.0).astype(jnp.bfloat16)


def block_scale(own_key, extent, cuts, low, top_value):
    def one(position, blocks):
        steps = jax.random.uniform(jax.random.fold_in(jax.random.fold_in(own_key, 6), position), (blocks,), jnp.float32, low / len(cuts), top_value / len(cuts))
        return jnp.repeat(jnp.exp(steps), extent[position] // blocks).reshape((-1,) + (1,) * (len(extent) - position - 1))

    level = one(*cuts[0])
    for cut in cuts[1:]:
        level = level * one(*cut)
    return level


def centred(key, dims, width, most, cuts=(), dtype=jnp.bfloat16):
    level = block_scale(key, dims, cuts, -0.22, 0.18) if cuts else 1.0
    values = jax.random.normal(key, dims, jnp.float32) * width * level
    return jnp.minimum(jnp.maximum(values, -most), most).astype(dtype)


def setup_inputs(seed: int = 0, part: int = 0) -> dict:
    key_of = jax.random.split(jax.random.key(seed), 11)
    own_keys = jax.random.split(jax.random.fold_in(key_of[10], part), 11)
    return {
        "tokens": draw_tokens(jax.random.fold_in(jax.random.fold_in(key_of[10], part), 71), part),
        "norm_gain": jnp.clip(1.0 + 0.18 * jax.random.normal(key_of[1], (2, D), jnp.float32), 0.1, 1.9),
        "w_query": centred(key_of[2], (2, D, DH), D ** -0.5, 0.09375, ((1, 32), (2, 16))),
        "w_forget": centred(key_of[3], (2, D, DH), D ** -0.5, 0.09375, ((1, 32), (2, 16))),
        "w_value": centred(key_of[4], (2, D, DH), D ** -0.5, 0.09375, ((1, 32), (2, 16))),
        "w_gate": centred(key_of[5], (2, D, DH), D ** -0.5, 0.09375, ((1, 32), (2, 16))),
        "lower_bound": jnp.clip(0.9 * jax.random.uniform(key_of[6], (2, DH), jnp.float32) ** block_scale(key_of[6], (2, DH), ((1, 16),), -0.2, 0.2), 0.0, 0.9),
        "head_gain": jnp.clip(1.0 + 0.18 * jax.random.normal(key_of[7], (2, HD), jnp.float32), 0.1, 1.9),
        "w_out": centred(key_of[8], (2, DH, D), DH ** -0.5, 0.125, ((1, 16), (2, 32))),
        "state": centred(own_keys[9], (2, BATCH, HEADS, HD, HD), 0.5, 4.0, ((1, 32), (2, 16)), jnp.float32),
    }


def reference(tokens, norm_gain, w_query, w_forget, w_value, w_gate, lower_bound, head_gain, w_out, state):
    hidden = tokens
    updated = []
    for layer in range(2):
        widened = hidden.astype(jnp.float32)
        factor = lax.rsqrt(lax.optimization_barrier(jnp.mean(widened * widened, axis=1, keepdims=True)) + 1e-06)
        scaled = (widened * norm_gain[layer]).astype(jnp.bfloat16)
        query = jnp.dot(scaled, w_query[layer], preferred_element_type=jnp.float32) * factor
        forget_pre = jnp.dot(scaled, w_forget[layer], preferred_element_type=jnp.float32) * factor
        value = jnp.dot(scaled, w_value[layer], preferred_element_type=jnp.float32) * factor
        gate_pre = jnp.dot(scaled, w_gate[layer], preferred_element_type=jnp.float32) * factor
        bound = lower_bound[layer]
        forget = bound + (1.0 - bound) * jax.nn.sigmoid(forget_pre)
        keyvec = (1.0 - bound) * jax.nn.sigmoid(-forget_pre)
        count = hidden.shape[0]
        head_count = query.shape[1] // HD
        shaped = lambda arr: arr.reshape(count, head_count, HD)
        carried = shaped(forget)[..., None] * state[layer] + shaped(keyvec)[..., None] * shaped(value)[..., None, :]
        updated.append(carried)
        readout = jnp.einsum('bhkv,bhk->bhv', carried, shaped(query))
        readout = readout * lax.rsqrt(lax.optimization_barrier(jnp.mean(readout * readout, axis=-1, keepdims=True)) + 1e-06) * head_gain[layer]
        normed = (readout.reshape(count, head_count * HD) * jax.nn.sigmoid(gate_pre)).astype(jnp.bfloat16)
        mixed = jnp.dot(normed, w_out[layer], preferred_element_type=jnp.float32)
        hidden = (widened + mixed).astype(jnp.bfloat16)
    return (hidden, jnp.stack(updated))
```

```python
import jax
import jax.numpy as jnp
from jax import lax
from jax.sharding import Mesh, PartitionSpec as P

D = 4096
HD = 128
NEAR = 4
BF16 = jnp.bfloat16
F32 = jnp.float32


def exchange(x, axis, groups=None):
    return lax.all_to_all(x, axis, 0, 0, tiled=True, axis_index_groups=groups)


def dot(a, b):
    return jnp.dot(a, b, preferred_element_type=F32)


def per_device(
    tokens, norm_gain, w_query, w_forget, w_value, w_gate, lower_bound, head_gain, w_out, state
):
    rows, width = tokens.shape
    local_seqs, head_count = state.shape[1:3]
    tp_size, y_size, c_size = (lax.axis_size(a) for a in ("tp", "y", "c"))
    assert c_size == 2 and rows == c_size * local_seqs and tp_size == y_size
    tp, core = lax.axis_index("tp"), lax.axis_index("c")
    held = y_size * local_seqs

    sent = jnp.broadcast_to(
        tokens.reshape(1, c_size, local_seqs, width), (tp_size, c_size, local_seqs, width)
    )
    got = exchange(sent.reshape(tp_size * c_size, local_seqs, width), ("tp", "c"))
    got = got.reshape(tp_size, c_size, local_seqs, width)
    own = jnp.where(core == 0, got[:, 0], got[:, 1]).reshape(held, width)
    mate = jnp.where(core == 0, got[:, 1], got[:, 0]).reshape(held, width)

    joined = jnp.concatenate([w_query, w_forget, w_value, w_gate], axis=2)
    joined = (joined.astype(F32) * norm_gain[:, :, None]).astype(BF16)
    packed = jnp.concatenate([joined, w_out], axis=2)
    other = lax.ppermute(packed, "c", [(0, 1), (1, 0)])
    proj_width = joined.shape[2]

    updated = []
    for layer in range(2):
        own_f, mate_f = own.astype(F32), mate.astype(F32)
        squares = jnp.sum(own_f * own_f + mate_f * mate_f, axis=1, keepdims=True)
        partial = dot(own, packed[layer, :, :proj_width]) + dot(mate, other[layer, :, :proj_width])
        payload = jnp.concatenate([partial.astype(BF16), squares.astype(BF16)], axis=1)
        got = exchange(payload.reshape(y_size, local_seqs, proj_width + 1), "y")
        total = jnp.sum(got.astype(F32), axis=0)
        factor = lax.rsqrt(total[:, proj_width:] / D + 1e-06)
        head_width = proj_width // 4
        query, forget_pre, value, gate_pre = (
            total[:, k * head_width : (k + 1) * head_width] * factor for k in range(4)
        )
        bound = lower_bound[layer]
        forget = bound + (1.0 - bound) * jax.nn.sigmoid(forget_pre)
        keyvec = (1.0 - bound) * jax.nn.sigmoid(-forget_pre)

        def shaped(array):
            return array.reshape(local_seqs, head_count, HD)

        carried = (
            shaped(forget)[..., None] * state[layer]
            + shaped(keyvec)[..., None] * shaped(value)[..., None, :]
        )
        updated.append(carried)
        readout = jnp.einsum("bhkv,bhk->bhv", carried, shaped(query))
        readout = (
            readout
            * lax.rsqrt(jnp.mean(readout * readout, axis=-1, keepdims=True) + 1e-06)
            * head_gain[layer]
        )
        normed = (readout.reshape(local_seqs, head_count * HD) * jax.nn.sigmoid(gate_pre)).astype(
            BF16
        )
        got = exchange(jnp.broadcast_to(normed[None], (y_size, *normed.shape)), "y")
        gathered = got.reshape(held, head_count * HD)
        mixed_own = dot(gathered, packed[layer, :, proj_width:])
        mixed_mate = dot(gathered, other[layer, :, proj_width:])
        if layer == 0:
            near = min(NEAR, tp_size)
            groups = [[j * near + i for i in range(near)] for j in range(tp_size // near)]
            mixed = jnp.concatenate([mixed_own, mixed_mate], axis=1).astype(BF16)
            got = exchange(mixed.reshape(near, held // near, 2 * width), "tp", groups)
            piece = jnp.sum(got.astype(F32), axis=0).astype(BF16)
            got = exchange(jnp.broadcast_to(piece[None], (tp_size, *piece.shape)), "tp")
            got = got.reshape(tp_size // near, near, held // near, 2 * width)
            mixed = jnp.sum(got.astype(F32), axis=0).reshape(held, 2 * width)
            own = (own_f + mixed[:, :width]).astype(BF16)
            mate = (mate_f + mixed[:, width:]).astype(BF16)
        else:
            mine = (jnp.arange(held) // local_seqs == tp)[:, None]
            mixed_own = (mixed_own + jnp.where(mine, own_f, 0.0)).astype(BF16)
            mixed_mate = (mixed_mate + jnp.where(mine, mate_f, 0.0)).astype(BF16)
            first = jnp.where(core == 0, mixed_own, mixed_mate)
            second = jnp.where(core == 0, mixed_mate, mixed_own)
            sent = jnp.stack(
                [a.reshape(tp_size, local_seqs, width) for a in (first, second)], axis=1
            )
            got = exchange(sent.reshape(tp_size * c_size, local_seqs, width), ("tp", "c"))
            got = got.reshape(tp_size, rows, width)
            hidden = jnp.sum(got.astype(F32), axis=0).astype(BF16)
    return (hidden, jnp.stack(updated))


def solution(mesh):
    grp, tp, dp = mesh.devices.shape
    fine = Mesh(mesh.devices.reshape(grp, tp, dp // 2, 2), ("grp", "tp", "y", "c"))
    dps = ("y", "c")
    weight = P(None, dps, "tp")
    held = P(None, ("grp", *dps), "tp", None, None)
    return jax.shard_map(
        per_device,
        mesh=fine,
        in_specs=(
            P(("grp", "tp"), dps),
            P(None, dps),
            weight,
            weight,
            weight,
            weight,
            P(None, "tp"),
            P(),
            P(None, "tp", dps),
            held,
        ),
        out_specs=(P(("grp", "tp"), dps), held),
        check_vma=False,
    )
```

```python
import jax
import jax.numpy as jnp
from jax import lax
from jax.sharding import Mesh, PartitionSpec as P

D = 4096
HD = 128
NEAR = 4
BF16 = jnp.bfloat16
F32 = jnp.float32


def exchange(x, axis, groups=None):
    return lax.all_to_all(x, axis, 0, 0, tiled=True, axis_index_groups=groups)


def dot(a, b):
    return jnp.dot(a, b, preferred_element_type=F32)


def per_device(
    tokens, norm_gain, w_query, w_forget, w_value, w_gate, lower_bound, head_gain, w_out, state
):
    rows, width = tokens.shape
    local_seqs, head_count = state.shape[1:3]
    tp_size, y_size, c_size = (lax.axis_size(a) for a in ("tp", "y", "c"))
    assert c_size == 2 and rows == c_size * local_seqs and tp_size == y_size
    tp, core = lax.axis_index("tp"), lax.axis_index("c")
    held = y_size * local_seqs

    sent = jnp.broadcast_to(
        tokens.reshape(1, c_size, local_seqs, width), (tp_size, c_size, local_seqs, width)
    )
    got = exchange(sent.reshape(tp_size * c_size, local_seqs, width), ("tp", "c"))
    got = got.reshape(tp_size, c_size, local_seqs, width)
    own = jnp.where(core == 0, got[:, 0], got[:, 1]).reshape(held, width)
    mate = jnp.where(core == 0, got[:, 1], got[:, 0]).reshape(held, width)

    joined = jnp.concatenate([w_query, w_forget, w_value, w_gate], axis=2)
    joined = (joined.astype(F32) * norm_gain[:, :, None]).astype(BF16)
    packed = jnp.concatenate([joined, w_out], axis=2)
    other = lax.ppermute(packed, "c", [(0, 1), (1, 0)])
    proj_width = joined.shape[2]

    mine = (lax.broadcasted_iota(jnp.int32, (held, width), 0) // local_seqs == tp).astype(F32)
    bounds = [jnp.broadcast_to(lower_bound[k], (local_seqs, lower_bound.shape[1])) for k in range(2)]
    gains = [jnp.broadcast_to(head_gain[k], (local_seqs, head_count, HD)) for k in range(2)]
    own, mate, mine, bounds, gains = lax.optimization_barrier((own, mate, mine, bounds, gains))

    updated = []
    for layer in range(2):
        own_f, mate_f = own.astype(F32), mate.astype(F32)
        squares = jnp.sum(own_f * own_f + mate_f * mate_f, axis=1, keepdims=True)
        partial = dot(own, packed[layer, :, :proj_width]) + dot(mate, other[layer, :, :proj_width])
        payload = jnp.concatenate([partial.astype(BF16), squares.astype(BF16)], axis=1)
        got = exchange(payload.reshape(y_size, local_seqs, proj_width + 1), "y")
        total = jnp.sum(got.astype(F32), axis=0)
        factor = lax.rsqrt(total[:, proj_width:] / D + 1e-06)
        head_width = proj_width // 4
        query, forget_pre, value, gate_pre = (
            total[:, k * head_width : (k + 1) * head_width] * factor for k in range(4)
        )
        bound = bounds[layer]
        forget = bound + (1.0 - bound) * jax.nn.sigmoid(forget_pre)
        keyvec = (1.0 - bound) * jax.nn.sigmoid(-forget_pre)

        def shaped(array):
            return array.reshape(local_seqs, head_count, HD)

        def advance(forget, keyvec, value, layer=layer):
            return (
                shaped(forget)[..., None] * state[layer]
                + shaped(keyvec)[..., None] * shaped(value)[..., None, :]
            )

        carried = advance(forget, keyvec, value)
        updated.append((advance, (forget, keyvec, value)))
        readout = jnp.einsum("bhkv,bhk->bhv", carried, shaped(query))
        readout = (
            readout
            * lax.rsqrt(jnp.mean(readout * readout, axis=-1, keepdims=True) + 1e-06)
            * gains[layer]
        )
        normed = (readout.reshape(local_seqs, head_count * HD) * jax.nn.sigmoid(gate_pre)).astype(
            BF16
        )
        got = exchange(jnp.broadcast_to(normed[None], (y_size, *normed.shape)), "y")
        if layer == 1:
            got, parts = lax.optimization_barrier((got, [p for _, p in updated]))
            updated = [form(*p) for (form, _), p in zip(updated, parts)]
        gathered = got.reshape(held, head_count * HD)
        mixed_own = dot(gathered, packed[layer, :, proj_width:])
        mixed_mate = dot(gathered, other[layer, :, proj_width:])
        if layer == 0:
            near = min(NEAR, tp_size)
            groups = [[j * near + i for i in range(near)] for j in range(tp_size // near)]
            mixed = jnp.concatenate([mixed_own, mixed_mate], axis=1).astype(BF16)
            got = exchange(mixed.reshape(near, held // near, 2 * width), "tp", groups)
            piece = jnp.sum(got.astype(F32), axis=0).astype(BF16)
            got = exchange(jnp.broadcast_to(piece[None], (tp_size, *piece.shape)), "tp")
            got = got.reshape(tp_size // near, near, held // near, 2 * width)
            mixed = jnp.sum(got.astype(F32), axis=0).reshape(held, 2 * width)
            own = (own_f + mixed[:, :width]).astype(BF16)
            mate = (mate_f + mixed[:, width:]).astype(BF16)
        else:
            mixed_own = (mixed_own + mine * own_f).astype(BF16)
            mixed_mate = (mixed_mate + mine * mate_f).astype(BF16)
            first = jnp.where(core == 0, mixed_own, mixed_mate)
            second = jnp.where(core == 0, mixed_mate, mixed_own)
            sent = jnp.stack(
                [a.reshape(tp_size, local_seqs, width) for a in (first, second)], axis=1
            )
            got = exchange(sent.reshape(tp_size * c_size, local_seqs, width), ("tp", "c"))
            got = got.reshape(tp_size, rows, width)
            hidden = jnp.sum(got.astype(F32), axis=0).astype(BF16)
    return (hidden, jnp.stack(updated))


def solution(mesh):
    grp, tp, dp = mesh.devices.shape
    fine = Mesh(mesh.devices.reshape(grp, tp, dp // 2, 2), ("grp", "tp", "y", "c"))
    dps = ("y", "c")
    weight = P(None, dps, "tp")
    held = P(None, ("grp", *dps), "tp", None, None)
    return jax.shard_map(
        per_device,
        mesh=fine,
        in_specs=(
            P(("grp", "tp"), dps),
            P(None, dps),
            weight,
            weight,
            weight,
            weight,
            P(None, "tp"),
            P(),
            P(None, "tp", dps),
            held,
        ),
        out_specs=(P(("grp", "tp"), dps), held),
        check_vma=False,
    )
```

```python
import jax
import jax.numpy as jnp
from jax import lax
from jax.sharding import Mesh, PartitionSpec as P

D = 4096
HD = 128
NEAR = 2
TP = ("far", "near")
BF16 = jnp.bfloat16
F32 = jnp.float32


def exchange(x, axis):
    return lax.all_to_all(x, axis, 0, 0, tiled=True)


def dot(a, b):
    return jnp.dot(a, b, preferred_element_type=F32)


def per_device(
    tokens, norm_gain, w_query, w_forget, w_value, w_gate, lower_bound, head_gain, w_out, state
):
    rows, width = tokens.shape
    local_seqs, head_count = state.shape[1:3]
    tp_size, y_size, c_size = (lax.axis_size(a) for a in (TP, "y", "c"))
    assert c_size == 2 and rows == c_size * local_seqs and tp_size == y_size
    tp, core, side = (lax.axis_index(a) for a in (TP, "c", "near"))
    held = y_size * local_seqs

    sent = jnp.broadcast_to(
        tokens.reshape(1, c_size, local_seqs, width), (tp_size, c_size, local_seqs, width)
    )
    got = exchange(sent.reshape(tp_size * c_size, local_seqs, width), (*TP, "c"))
    got = got.reshape(tp_size, c_size, local_seqs, width)
    own = jnp.where(core == 0, got[:, 0], got[:, 1]).reshape(held, width)
    mate = jnp.where(core == 0, got[:, 1], got[:, 0]).reshape(held, width)

    joined = jnp.concatenate([w_query, w_forget, w_value, w_gate], axis=2)
    joined = (joined.astype(F32) * norm_gain[:, :, None]).astype(BF16)
    packed = jnp.concatenate([joined, w_out], axis=2)
    other = lax.ppermute(packed, "c", [(0, 1), (1, 0)])
    proj_width = joined.shape[2]

    pair_out = jnp.concatenate([w_out[0], other[0, :, proj_width:]], axis=1)
    near_out = lax.ppermute(pair_out, "near", [(0, 1), (1, 0)])

    mine = (lax.broadcasted_iota(jnp.int32, (held, width), 0) // local_seqs == tp).astype(F32)
    bounds = [jnp.broadcast_to(lower_bound[k], (local_seqs, lower_bound.shape[1])) for k in range(2)]
    gains = [jnp.broadcast_to(head_gain[k], (local_seqs, head_count, HD)) for k in range(2)]
    own, mate, mine, bounds, gains, pair_out, near_out, side = lax.optimization_barrier(
        (own, mate, mine, bounds, gains, pair_out, near_out, side)
    )

    updated = []
    for layer in range(2):
        own_f, mate_f = own.astype(F32), mate.astype(F32)
        squares = jnp.sum(own_f * own_f + mate_f * mate_f, axis=1, keepdims=True)
        partial = dot(own, packed[layer, :, :proj_width]) + dot(mate, other[layer, :, :proj_width])
        payload = jnp.concatenate([partial.astype(BF16), squares.astype(BF16)], axis=1)
        got = exchange(payload.reshape(y_size, local_seqs, proj_width + 1), "y")
        total = jnp.sum(got.astype(F32), axis=0)
        factor = lax.rsqrt(total[:, proj_width:] / D + 1e-06)
        head_width = proj_width // 4
        query, forget_pre, value, gate_pre = (
            total[:, k * head_width : (k + 1) * head_width] * factor for k in range(4)
        )
        bound = bounds[layer]
        forget = bound + (1.0 - bound) * jax.nn.sigmoid(forget_pre)
        keyvec = (1.0 - bound) * jax.nn.sigmoid(-forget_pre)

        def shaped(array):
            return array.reshape(local_seqs, head_count, HD)

        def advance(forget, keyvec, value, layer=layer):
            return (
                shaped(forget)[..., None] * state[layer]
                + shaped(keyvec)[..., None] * shaped(value)[..., None, :]
            )

        carried = advance(forget, keyvec, value)
        updated.append((advance, (forget, keyvec, value)))
        readout = jnp.einsum("bhkv,bhk->bhv", carried, shaped(query))
        readout = (
            readout
            * lax.rsqrt(jnp.mean(readout * readout, axis=-1, keepdims=True) + 1e-06)
            * gains[layer]
        )
        normed = (readout.reshape(local_seqs, head_count * HD) * jax.nn.sigmoid(gate_pre)).astype(
            BF16
        )
        if layer == 0:
            got = exchange(
                jnp.broadcast_to(normed[None], (NEAR * y_size, *normed.shape)), ("near", "y")
            ).reshape(NEAR, NEAR, held // NEAR, head_count * HD)
            part = jnp.where(side == 0, got[:, 0], got[:, 1])
            mixed = dot(jnp.where(side == 0, part[0], part[1]), pair_out)
            mixed = mixed + dot(jnp.where(side == 0, part[1], part[0]), near_out)
            piece = mixed.astype(BF16)
            got = exchange(jnp.broadcast_to(piece[None], (tp_size, *piece.shape)), TP)
            got = got.reshape(tp_size // NEAR, NEAR, held // NEAR, 2 * width)
            mixed = jnp.sum(got.astype(F32), axis=0).reshape(held, 2 * width)
            own = (own_f + mixed[:, :width]).astype(BF16)
            mate = (mate_f + mixed[:, width:]).astype(BF16)
        else:
            got = exchange(jnp.broadcast_to(normed[None], (y_size, *normed.shape)), "y")
            got, parts = lax.optimization_barrier((got, [p for _, p in updated]))
            updated = [form(*p) for (form, _), p in zip(updated, parts)]
            gathered = got.reshape(held, head_count * HD)
            mixed_own = dot(gathered, packed[layer, :, proj_width:])
            mixed_mate = dot(gathered, other[layer, :, proj_width:])
            mixed_own = (mixed_own + mine * own_f).astype(BF16)
            mixed_mate = (mixed_mate + mine * mate_f).astype(BF16)
            first = jnp.where(core == 0, mixed_own, mixed_mate)
            second = jnp.where(core == 0, mixed_mate, mixed_own)
            sent = jnp.stack(
                [a.reshape(tp_size, local_seqs, width) for a in (first, second)], axis=1
            )
            got = exchange(sent.reshape(tp_size * c_size, local_seqs, width), (*TP, "c"))
            got = got.reshape(tp_size, rows, width)
            hidden = jnp.sum(got.astype(F32), axis=0).astype(BF16)
    return (hidden, jnp.stack(updated))


def solution(mesh):
    grp, tp, dp = mesh.devices.shape
    fine = Mesh(
        mesh.devices.reshape(grp, tp // NEAR, NEAR, dp // 2, 2), ("grp", "far", "near", "y", "c")
    )
    tps, dps = ("far", "near"), ("y", "c")
    weight = P(None, dps, tps)
    held = P(None, ("grp", *dps), tps, None, None)
    return jax.shard_map(
        per_device,
        mesh=fine,
        in_specs=(
            P(("grp", *tps), dps),
            P(None, dps),
            weight,
            weight,
            weight,
            weight,
            P(None, tps),
            P(),
            P(None, tps, dps),
            held,
        ),
        out_specs=(P(("grp", *tps), dps), held),
        check_vma=False,
    )
```

```python
import jax
import jax.numpy as jnp
from jax import lax
from jax.sharding import Mesh, PartitionSpec as P

D = 4096
HD = 128
NEAR = 4
BF16 = jnp.bfloat16
F32 = jnp.float32


def exchange(x, axis, groups=None):
    return lax.all_to_all(x, axis, 0, 0, tiled=True, axis_index_groups=groups)


def dot(a, b):
    return jnp.dot(a, b, preferred_element_type=F32)


def per_device(
    tokens, norm_gain, w_query, w_forget, w_value, w_gate, lower_bound, head_gain, w_out, state
):
    rows, width = tokens.shape
    local_seqs, head_count = state.shape[1:3]
    tp_size, y_size, c_size = (lax.axis_size(a) for a in ("tp", "y", "c"))
    assert c_size == 2 and rows == c_size * local_seqs and tp_size == y_size
    tp, core = lax.axis_index("tp"), lax.axis_index("c")
    held = y_size * local_seqs

    sent = jnp.broadcast_to(
        tokens.reshape(1, c_size, local_seqs, width), (tp_size, c_size, local_seqs, width)
    )
    got = exchange(sent.reshape(tp_size * c_size, local_seqs, width), ("tp", "c"))
    got = got.reshape(tp_size, c_size, local_seqs, width)
    own = jnp.where(core == 0, got[:, 0], got[:, 1]).reshape(held, width)
    mate = jnp.where(core == 0, got[:, 1], got[:, 0]).reshape(held, width)

    joined = jnp.concatenate([w_query, w_forget, w_value, w_gate], axis=2)
    joined = (joined.astype(F32) * norm_gain[:, :, None]).astype(BF16)
    packed = jnp.concatenate([joined, w_out], axis=2)
    other = lax.ppermute(packed, "c", [(0, 1), (1, 0)])
    proj_width = joined.shape[2]

    mine = (lax.broadcasted_iota(jnp.int32, (held, width), 0) // local_seqs == tp).astype(F32)
    bounds = [jnp.broadcast_to(lower_bound[k], (local_seqs, lower_bound.shape[1])) for k in range(2)]
    gains = [jnp.broadcast_to(head_gain[k], (local_seqs, head_count, HD)) for k in range(2)]
    own, mate, mine, bounds, gains = lax.optimization_barrier((own, mate, mine, bounds, gains))

    steps = []
    for layer in range(2):
        own_f, mate_f = own.astype(F32), mate.astype(F32)
        squares = jnp.sum(own_f * own_f + mate_f * mate_f, axis=1, keepdims=True)
        partial = dot(own, packed[layer, :, :proj_width]) + dot(mate, other[layer, :, :proj_width])
        payload = jnp.concatenate([partial.astype(BF16), squares.astype(BF16)], axis=1)
        got = exchange(payload.reshape(y_size, local_seqs, proj_width + 1), "y")
        total = jnp.sum(got.astype(F32), axis=0)
        factor = lax.rsqrt(total[:, proj_width:] / D + 1e-06)
        head_width = proj_width // 4
        query, forget_pre, value, gate_pre = (
            total[:, k * head_width : (k + 1) * head_width] * factor for k in range(4)
        )
        bound = bounds[layer]
        forget = bound + (1.0 - bound) * jax.nn.sigmoid(forget_pre)
        keyvec = (1.0 - bound) * jax.nn.sigmoid(-forget_pre)

        def shaped(array):
            return array.reshape(local_seqs, head_count, HD)

        def advance(forget, keyvec, value, old):
            return forget[..., None] * old + keyvec[..., None] * value[..., None, :]

        step = [shaped(a) for a in (forget, keyvec, value)]
        steps.append(step)
        carried = advance(*step, state[layer])
        readout = jnp.einsum("bhkv,bhk->bhv", carried, shaped(query))
        readout = (
            readout
            * lax.rsqrt(jnp.mean(readout * readout, axis=-1, keepdims=True) + 1e-06)
            * gains[layer]
        )
        normed = (readout.reshape(local_seqs, head_count * HD) * jax.nn.sigmoid(gate_pre)).astype(
            BF16
        )
        got = exchange(jnp.broadcast_to(normed[None], (y_size, *normed.shape)), "y")
        gathered = got.reshape(held, head_count * HD)
        mixed_own = dot(gathered, packed[layer, :, proj_width:])
        mixed_mate = dot(gathered, other[layer, :, proj_width:])
        if layer == 0:
            near = min(NEAR, tp_size)
            groups = [[j * near + i for i in range(near)] for j in range(tp_size // near)]
            mixed = jnp.concatenate([mixed_own, mixed_mate], axis=1).astype(BF16)
            got = exchange(mixed.reshape(near, held // near, 2 * width), "tp", groups)
            piece = jnp.sum(got.astype(F32), axis=0).astype(BF16)
            got = exchange(jnp.broadcast_to(piece[None], (tp_size, *piece.shape)), "tp")
            got = got.reshape(tp_size // near, near, held // near, 2 * width)
            mixed = jnp.sum(got.astype(F32), axis=0).reshape(held, 2 * width)
            own = (own_f + mixed[:, :width]).astype(BF16)
            mate = (mate_f + mixed[:, width:]).astype(BF16)
        else:
            mixed_own = (mixed_own + mine * own_f).astype(BF16)
            mixed_mate = (mixed_mate + mine * mate_f).astype(BF16)
            first = jnp.where(core == 0, mixed_own, mixed_mate)
            second = jnp.where(core == 0, mixed_mate, mixed_own)
            sent = jnp.stack(
                [a.reshape(tp_size, local_seqs, width) for a in (first, second)], axis=1
            )
            got = exchange(sent.reshape(tp_size * c_size, local_seqs, width), ("tp", "c"))
            got, steps = lax.optimization_barrier((got, steps))
            got = got.reshape(tp_size, rows, width)
            hidden = jnp.sum(got.astype(F32), axis=0).astype(BF16)
    moved = advance(*(jnp.stack(pair) for pair in zip(*steps)), state)
    return (hidden, moved)


def solution(mesh):
    grp, tp, dp = mesh.devices.shape
    fine = Mesh(mesh.devices.reshape(grp, tp, dp // 2, 2), ("grp", "tp", "y", "c"))
    dps = ("y", "c")
    weight = P(None, dps, "tp")
    held = P(None, ("grp", *dps), "tp", None, None)
    return jax.shard_map(
        per_device,
        mesh=fine,
        in_specs=(
            P(("grp", "tp"), dps),
            P(None, dps),
            weight,
            weight,
            weight,
            weight,
            P(None, "tp"),
            P(),
            P(None, "tp", dps),
            held,
        ),
        out_specs=(P(("grp", "tp"), dps), held),
        check_vma=False,
    )
```

```python
import jax
import jax.numpy as jnp
from jax import lax
from jax.sharding import Mesh, PartitionSpec as P

D = 4096
HD = 128
NEAR = 4
BF16 = jnp.bfloat16
F32 = jnp.float32


def exchange(x, axis, groups=None):
    return lax.all_to_all(x, axis, 0, 0, tiled=True, axis_index_groups=groups)


def dot(a, b):
    return jnp.dot(a, b, preferred_element_type=F32)


def per_device(
    tokens, norm_gain, w_query, w_forget, w_value, w_gate, lower_bound, head_gain, w_out, state
):
    rows, width = tokens.shape
    local_seqs, head_count = state.shape[1:3]
    tp_size, y_size, c_size = (lax.axis_size(a) for a in ("tp", "y", "c"))
    assert c_size == 2 and rows == c_size * local_seqs and tp_size == y_size
    tp, core = lax.axis_index("tp"), lax.axis_index("c")
    held = y_size * local_seqs

    sent = jnp.broadcast_to(
        tokens.reshape(1, c_size, local_seqs, width), (tp_size, c_size, local_seqs, width)
    )
    got = exchange(sent.reshape(tp_size * c_size, local_seqs, width), ("tp", "c"))
    got = got.reshape(tp_size, c_size, local_seqs, width)
    parts = [got[:, k].reshape(held, width) for k in range(c_size)]

    joined = jnp.concatenate([w_query, w_forget, w_value, w_gate], axis=2)
    joined = (joined.astype(F32) * norm_gain[:, :, None]).astype(BF16)
    packed = jnp.concatenate([joined, w_out], axis=2)
    other = lax.ppermute(packed, "c", [(0, 1), (1, 0)])
    proj_width = joined.shape[2]
    ordered = [jnp.where(core == k, packed, other) for k in range(c_size)]

    mine = (lax.broadcasted_iota(jnp.int32, (held, width), 0) // local_seqs == tp).astype(F32)
    bounds = [jnp.broadcast_to(lower_bound[k], (local_seqs, lower_bound.shape[1])) for k in range(2)]
    gains = [jnp.broadcast_to(head_gain[k], (local_seqs, head_count, HD)) for k in range(2)]
    ones = jnp.ones((width, width), BF16)
    parts, mine, bounds, gains, ordered, ones = lax.optimization_barrier(
        (parts, mine, bounds, gains, ordered, ones)
    )

    steps = []
    for layer in range(2):
        wide = [part.astype(F32) for part in parts]
        squares = dot(sum(w * w for w in wide).astype(BF16), ones)
        partial = sum(dot(p, w[layer, :, :proj_width]) for p, w in zip(parts, ordered))
        payload = jnp.concatenate([partial.astype(BF16), squares.astype(BF16)], axis=1)
        got = exchange(payload.reshape(y_size, local_seqs, proj_width + width), "y")
        total = jnp.sum(got.astype(F32), axis=0)
        factor = lax.rsqrt(total[:, proj_width:] / D + 1e-06)
        head_width = proj_width // 4
        query, forget_pre, value, gate_pre = (
            total[:, k * head_width : (k + 1) * head_width] * factor for k in range(4)
        )
        bound = bounds[layer]
        forget = bound + (1.0 - bound) * jax.nn.sigmoid(forget_pre)
        keyvec = (1.0 - bound) * jax.nn.sigmoid(-forget_pre)

        def shaped(array):
            return array.reshape(local_seqs, head_count, HD)

        def advance(forget, keyvec, value, old):
            return forget[..., None] * old + keyvec[..., None] * value[..., None, :]

        step = [shaped(a) for a in (forget, keyvec, value)]
        steps.append(step)
        carried = advance(*step, state[layer])
        readout = jnp.einsum("bhkv,bhk->bhv", carried, shaped(query))
        readout = (
            readout
            * lax.rsqrt(jnp.mean(readout * readout, axis=-1, keepdims=True) + 1e-06)
            * gains[layer]
        )
        normed = (readout.reshape(local_seqs, head_count * HD) * jax.nn.sigmoid(gate_pre)).astype(
            BF16
        )
        got = exchange(jnp.broadcast_to(normed[None], (y_size, *normed.shape)), "y")
        gathered = got.reshape(held, head_count * HD)
        mixed = [dot(gathered, w[layer, :, proj_width:]) for w in ordered]
        if layer == 0:
            near = min(NEAR, tp_size)
            groups = [[j * near + i for i in range(near)] for j in range(tp_size // near)]
            mixed = jnp.concatenate(mixed, axis=1).astype(BF16)
            got = exchange(mixed.reshape(near, held // near, 2 * width), "tp", groups)
            piece = jnp.sum(got.astype(F32), axis=0).astype(BF16)
            got = exchange(jnp.broadcast_to(piece[None], (tp_size, *piece.shape)), "tp")
            got = got.reshape(tp_size // near, near, held // near, 2 * width)
            mixed = jnp.sum(got.astype(F32), axis=0).reshape(held, 2 * width)
            parts = [
                (w + mixed[:, k * width : (k + 1) * width]).astype(BF16) for k, w in enumerate(wide)
            ]
        else:
            sent = jnp.stack(
                [
                    (m + mine * w).astype(BF16).reshape(tp_size, local_seqs, width)
                    for m, w in zip(mixed, wide)
                ],
                axis=1,
            )
            got = exchange(sent.reshape(tp_size * c_size, local_seqs, width), ("tp", "c"))
            got, steps = lax.optimization_barrier((got, steps))
            got = got.reshape(tp_size, rows, width)
            hidden = jnp.sum(got.astype(F32), axis=0).astype(BF16)
    moved = advance(*(jnp.stack(pair) for pair in zip(*steps)), state)
    return (hidden, moved)


def solution(mesh):
    grp, tp, dp = mesh.devices.shape
    fine = Mesh(mesh.devices.reshape(grp, tp, dp // 2, 2), ("grp", "tp", "y", "c"))
    dps = ("y", "c")
    weight = P(None, dps, "tp")
    held = P(None, ("grp", *dps), "tp", None, None)
    return jax.shard_map(
        per_device,
        mesh=fine,
        in_specs=(
            P(("grp", "tp"), dps),
            P(None, dps),
            weight,
            weight,
            weight,
            weight,
            P(None, "tp"),
            P(),
            P(None, "tp", dps),
            held,
        ),
        out_specs=(P(("grp", "tp"), dps), held),
        check_vma=False,
    )
```

```python
import jax
import jax.numpy as jnp
from jax import lax
from jax.sharding import Mesh, PartitionSpec as P

D = 4096
HD = 128
NEAR = 4
BF16 = jnp.bfloat16
F32 = jnp.float32


def exchange(x, axis, groups=None):
    return lax.all_to_all(x, axis, 0, 0, tiled=True, axis_index_groups=groups)


def dot(a, b):
    return jnp.dot(a, b, preferred_element_type=F32)


def per_device(
    tokens, norm_gain, w_query, w_forget, w_value, w_gate, lower_bound, head_gain, w_out, state
):
    rows, width = tokens.shape
    local_seqs, head_count = state.shape[1:3]
    tp_size, y_size, c_size = (lax.axis_size(a) for a in ("tp", "y", "c"))
    assert c_size == 2 and rows == c_size * local_seqs and tp_size == y_size
    tp, core = lax.axis_index("tp"), lax.axis_index("c")
    held = y_size * local_seqs

    sent = jnp.broadcast_to(
        tokens.reshape(1, c_size, local_seqs, width), (tp_size, c_size, local_seqs, width)
    )
    got = exchange(sent.reshape(tp_size * c_size, local_seqs, width), ("tp", "c"))
    got = got.reshape(tp_size, c_size, local_seqs, width)
    hidden = jnp.concatenate([got[:, k].reshape(held, width) for k in range(c_size)], axis=1)

    joined = jnp.concatenate([w_query, w_forget, w_value, w_gate], axis=2)
    joined = (joined.astype(F32) * norm_gain[:, :, None]).astype(BF16)
    packed = jnp.concatenate([joined, w_out], axis=2)
    other = lax.ppermute(packed, "c", [(0, 1), (1, 0)])
    proj_width = joined.shape[2]
    ordered = [jnp.where(core == k, packed, other) for k in range(c_size)]
    w_proj = jnp.concatenate([w[:, :, :proj_width] for w in ordered], axis=1)
    w_mix = jnp.concatenate([w[:, :, proj_width:] for w in ordered], axis=2)

    mine = (lax.broadcasted_iota(jnp.int32, (held, c_size * width), 0) // local_seqs == tp).astype(F32)
    bounds = [jnp.broadcast_to(lower_bound[k], (local_seqs, lower_bound.shape[1])) for k in range(2)]
    gains = [jnp.broadcast_to(head_gain[k], (local_seqs, head_count, HD)) for k in range(2)]
    ones = jnp.ones((c_size * width, width), BF16)
    hidden, mine, bounds, gains, w_proj, w_mix, ones = lax.optimization_barrier(
        (hidden, mine, bounds, gains, w_proj, w_mix, ones)
    )

    steps = []
    for layer in range(2):
        wide = hidden.astype(F32)
        squares = dot((wide * wide).astype(BF16), ones)
        partial = dot(hidden, w_proj[layer])
        payload = jnp.concatenate([partial.astype(BF16), squares.astype(BF16)], axis=1)
        got = exchange(payload.reshape(y_size, local_seqs, proj_width + width), "y")
        total = jnp.sum(got.astype(F32), axis=0)
        factor = lax.rsqrt(total[:, proj_width:] / D + 1e-06)
        head_width = proj_width // 4
        query, forget_pre, value, gate_pre = (
            total[:, k * head_width : (k + 1) * head_width] * factor for k in range(4)
        )
        bound = bounds[layer]
        forget = bound + (1.0 - bound) * jax.nn.sigmoid(forget_pre)
        keyvec = (1.0 - bound) * jax.nn.sigmoid(-forget_pre)

        def shaped(array):
            return array.reshape(local_seqs, head_count, HD)

        def advance(forget, keyvec, value, old):
            return forget[..., None] * old + keyvec[..., None] * value[..., None, :]

        step = [shaped(a) for a in (forget, keyvec, value)]
        steps.append(step)
        carried = advance(*step, state[layer])
        readout = jnp.einsum("bhkv,bhk->bhv", carried, shaped(query))
        readout = (
            readout
            * lax.rsqrt(dot((readout * readout).astype(BF16), ones[:HD, :HD]) / HD + 1e-06)
            * gains[layer]
        )
        normed = (readout.reshape(local_seqs, head_count * HD) * jax.nn.sigmoid(gate_pre)).astype(
            BF16
        )
        got = exchange(jnp.broadcast_to(normed[None], (y_size, *normed.shape)), "y")
        if layer == 1:
            got, steps = lax.optimization_barrier((got, steps))
        gathered = got.reshape(held, head_count * HD)
        mixed = dot(gathered, w_mix[layer])
        if layer == 0:
            near = min(NEAR, tp_size)
            groups = [[j * near + i for i in range(near)] for j in range(tp_size // near)]
            mixed = mixed.astype(BF16)
            got = exchange(mixed.reshape(near, held // near, 2 * width), "tp", groups)
            piece = jnp.sum(got.astype(F32), axis=0).astype(BF16)
            got = exchange(jnp.broadcast_to(piece[None], (tp_size, *piece.shape)), "tp")
            got = got.reshape(tp_size // near, near, held // near, 2 * width)
            mixed = jnp.sum(got.astype(F32), axis=0).reshape(held, 2 * width)
            hidden = (wide + mixed).astype(BF16)
        else:
            sent = (mixed + mine * wide).astype(BF16)
            sent = jnp.swapaxes(sent.reshape(tp_size, local_seqs, c_size, width), 1, 2)
            got = exchange(sent.reshape(tp_size * c_size, local_seqs, width), ("tp", "c"))
            got = got.reshape(tp_size, rows, width)
            hidden = jnp.sum(got.astype(F32), axis=0).astype(BF16)
    moved = advance(*(jnp.stack(pair) for pair in zip(*steps)), state)
    return (hidden, moved)


def solution(mesh):
    grp, tp, dp = mesh.devices.shape
    fine = Mesh(mesh.devices.reshape(grp, tp, dp // 2, 2), ("grp", "tp", "y", "c"))
    dps = ("y", "c")
    weight = P(None, dps, "tp")
    held = P(None, ("grp", *dps), "tp", None, None)
    return jax.shard_map(
        per_device,
        mesh=fine,
        in_specs=(
            P(("grp", "tp"), dps),
            P(None, dps),
            weight,
            weight,
            weight,
            weight,
            P(None, "tp"),
            P(),
            P(None, "tp", dps),
            held,
        ),
        out_specs=(P(("grp", "tp"), dps), held),
        check_vma=False,
    )
```
